1024 devices in a mesh: ep: 64 (over z, core), tp: 16 (over y, x).
Axes of the slice: x: 4, y: 4, z: 32, core: 2. Of those that a mesh axis runs over, the one named last changes fastest.
Arguments:
- tokens: bfloat16 [8192, 2048], P('ep', 'tp'), may hold values from -6 to 6
- routing: int32 [8192, 2], P('ep'), may hold values from 0 to 31, all different within a row; in each aligned block of 128 rows (0 to 127, 128 to 255, ...) at most 10 rows name the same one
- mixing: float32 [8192, 2], P('ep'), may hold values from 0.1 to 0.9
- gate_matrix: bfloat16 [64, 2048, 2048], P('ep', None, 'tp'), may hold values from -0.125 to 0.125
- up_matrix: bfloat16 [64, 2048, 2048], P('ep', None, 'tp'), may hold values from -0.125 to 0.125
- down_matrix: bfloat16 [64, 2048, 2048], P('ep', 'tp'), may hold values from -0.09375 to 0.09375
- upstream: bfloat16 [8192, 2048], P('ep', 'tp'), may hold values from -6 to 6
Outputs:
- token_gradient: bfloat16 [8192, 2048], P('ep', 'tp')
- mixing_gradient: float32 [8192, 2], P('ep')
- gate_gradient: bfloat16 [64, 2048, 2048], P('ep', None, 'tp')
- up_gradient: bfloat16 [64, 2048, 2048], P('ep', None, 'tp')
- down_gradient: bfloat16 [64, 2048, 2048], P('ep', 'tp')
- input_norms: float32 [64, 2, 2048], P('ep')
- down_norms: float32 [64, 2048], P('ep', 'tp')
The draws below stay inside these ranges and needn't reach their ends.
Inputs may be any that keep to these rules, and one draw needn't show every extreme that they name: `routing`: A token's 2 experts differ. In each aligned block of 128 rows (the rows of one index of ep) no expert is named by more than 10 rows, and in every draw some expert is named by exactly 10 rows of some block.
All inputs are finite; a program needn't handle non-finite values.
Results may differ from the reference program's by a relative error of at most 0.0064.
Values may be sent and summed in bfloat16 or wider, within the bound.
A program may use at most 64 MiB of HBM per device.

```python
import math
from functools import partial
import jax
import jax.numpy as jnp
import numpy as np
from jax import lax

D = 2048
FF = 4096
TOP = 2
TOK_DEV = 128
EXPERTS = 32
SLABS = 64
FF_HALF = 2048
CAP = 10
TOKENS = 8192
N_EP = 64
N_TP = 16


def levels(rng, extent, pieces, least, high):
    loudness = 1.0
    for axis_at, blocks in pieces:
        steps = jax.random.uniform(jax.random.fold_in(jax.random.fold_in(rng, 6), axis_at), (blocks,), jnp.float32, least / len(pieces), high / len(pieces))
        loudness = loudness * jnp.repeat(jnp.exp(steps), extent[axis_at] // blocks).reshape((-1,) + (1,) * (len(extent) - 1 - axis_at))
    return loudness


def routed_block(own_key, own, number, rows, count, top, bound, lean):
    ranking = jax.random.permutation(own_key, count)
    packed, common = shares(count, rows * top, bound, lean, True), shares(count, rows * top, bound, lean, False)
    places = jnp.arange(count)

    def named(lengths, turn):
        used = int((lengths > 0).sum())
        fixed = max(1, used // 4)
        shifted = fixed + (places - fixed + turn * (used - fixed)) % max(1, count - fixed)
        return jnp.zeros((count,), jnp.int32).at[ranking[jnp.where(places < fixed, places, shifted)]].set(jnp.asarray(lengths, jnp.int32))

    lengths = jnp.where(number % 4 == 0, named(packed, number // 4), named(common, number - number // 4 - 1))
    mixed = jax.random.permutation(jax.random.fold_in(own, 3), count)
    source_of, receiver = mixed[0:count // 2 * 2:2], mixed[1:count // 2 * 2:2]
    slack = jnp.minimum(lengths[source_of] - 1, bound - lengths[receiver]) // 2
    slack = jnp.where((source_of == ranking[0]) | (receiver == ranking[0]) | (lengths[receiver] == 0), 0, jnp.maximum(slack, 0))
    shifted = jax.random.randint(jax.random.fold_in(own, 4), (count // 2,), 0, 1 << 20) % (slack + 1)
    lengths = lengths.at[source_of].add(-shifted).at[receiver].add(shifted)
    members = jnp.searchsorted(jnp.cumsum(lengths), jnp.arange(rows * top), side="right").astype(jnp.int32)
    listing = members.reshape(top, rows).T
    listing = listing[jax.random.permutation(jax.random.fold_in(own, 1), rows)]
    turn = jax.random.randint(jax.random.fold_in(own, 2), (rows, 1), 0, top)
    return jnp.take_along_axis(listing, (jnp.arange(top)[None, :] + turn) % top, axis=1)


def shares(amount, total, most, skew, full):
    loads = [(1 << 20) // math.isqrt(rank ** skew) + 1 for rank in range(1, amount + 1)]
    largest = most if full else min(most, max(-(-total // amount), total * loads[0] // sum(loads)))
    least = 1 if total - largest >= amount - 1 else 0
    given, spare = [largest] + [least] * (amount - 1), total - largest - least * (amount - 1)
    while spare > 0:
        candidates = [i for i in range(1, amount) if given[i] < largest] or [i for i in range(1, amount) if given[i] < most]
        whole, budget = sum([loads[i] for i in candidates]), spare
        for i in candidates:
            addition = min(most - given[i], max(1, budget * loads[i] // whole), spare)
            given[i] = given[i] + addition
            spare = spare - addition
    return np.array(given)


def noise(own_key, extent, width, most, cuts=(), held_as=jnp.bfloat16):
    result = jax.random.normal(own_key, extent, jnp.float32) * width
    if len(cuts) > 0:
        result = levels(own_key, extent, cuts, -0.22, 0.18) * result
    return jnp.clip(result, min=-most, max=most).astype(held_as)


def setup_inputs(seed: int = 0) -> dict:
    key_list = jax.random.split(jax.random.key(seed), 8)
    tokens = noise(key_list[0], (TOKENS, D), 1.0, 6.0, ((0, 64), (1, 16)))
    routing_keys = jax.random.split(jax.random.fold_in(key_list[1], 1), TOKENS // TOK_DEV)
    routing_turns = jax.random.permutation(jax.random.fold_in(key_list[1], 3), TOKENS // TOK_DEV)
    routing = jax.vmap(lambda own, number: routed_block(jax.random.fold_in(key_list[1], 2), own, number, TOK_DEV, EXPERTS, TOP, CAP, 1))(routing_keys, routing_turns).reshape((TOKENS, TOP))
    mixing = jnp.clip(0.1 + 0.79999997 * jax.random.uniform(key_list[2], (TOKENS, TOP), jnp.float32) ** levels(key_list[2], (TOKENS, TOP), ((0, 64),), -0.2, 0.2), 0.1, 0.9)
    gate_matrix = noise(key_list[3], (SLABS, D, FF_HALF), D ** -0.5, 0.125, ((0, 64), (2, 16)))
    up_matrix = noise(key_list[4], (SLABS, D, FF_HALF), D ** -0.5, 0.125, ((0, 64), (2, 16)))
    down_matrix = noise(key_list[5], (SLABS, FF_HALF, D), FF ** -0.5, 0.09375, ((0, 64), (1, 16)))
    upstream = noise(key_list[6], (TOKENS, D), 1.0, 6.0, ((0, 64), (1, 16)))
    return dict(tokens=tokens, routing=routing, mixing=mixing, gate_matrix=gate_matrix, up_matrix=up_matrix, down_matrix=down_matrix, upstream=upstream)


def slot_targets(route_block, experts, capacity):
    flat_routes = route_block.reshape(-1).astype(jnp.int32)
    choose = (flat_routes[:, None] == jnp.arange(experts, dtype=jnp.int32)[None, :]).astype(jnp.int32)
    earlier = jnp.cumsum(choose, axis=0) - choose
    return (flat_routes * capacity + jnp.sum(earlier * choose, axis=1)).astype(jnp.int32)


def place_rows(target, values, slot_count):
    matches = (target[:, None] == jnp.arange(slot_count, dtype=jnp.int32)[None, :]).astype(values.dtype)
    placed = lax.dot_general(matches, values, (((0,), (0,)), ((), ())), preferred_element_type=jnp.float32)
    return placed.astype(jnp.bfloat16)


def take_rows(values, target):
    return jnp.take(values, target, axis=0)


def expert_backward(token_rows, grad_rows, gate_mat, up_mat, down_mat):
    gate_pre = jnp.dot(token_rows, gate_mat, preferred_element_type=jnp.float32)
    up_pre = jnp.dot(token_rows, up_mat, preferred_element_type=jnp.float32)
    sigmoid_gate = jax.nn.sigmoid(gate_pre)
    activated = gate_pre * sigmoid_gate
    hidden = activated * up_pre
    back_grad = lax.dot_general(grad_rows, down_mat, (((1,), (1,)), ((), ())), preferred_element_type=jnp.float32)
    up_grad = (back_grad * activated).astype(jnp.bfloat16)
    gate_grad = (back_grad * up_pre * sigmoid_gate * (1.0 + gate_pre * (1.0 - sigmoid_gate))).astype(jnp.bfloat16)
    hidden_low = hidden.astype(jnp.bfloat16)
    contract_rows = (((0,), (0,)), ((), ()))
    down_full = lax.dot_general(hidden_low, grad_rows, contract_rows, preferred_element_type=jnp.float32)
    gate_full = lax.dot_general(token_rows, gate_grad, contract_rows, preferred_element_type=jnp.float32)
    up_full = lax.dot_general(token_rows, up_grad, contract_rows, preferred_element_type=jnp.float32)
    scores = jnp.sum(hidden * back_grad, axis=1)
    return gate_full, up_full, down_full, gate_grad, up_grad, scores


def reference(tokens, routing, mixing, gate_matrix, up_matrix, down_matrix, upstream):
    sources = N_EP
    slot_count = EXPERTS * CAP
    route_blocks = routing.reshape(sources, TOK_DEV, TOP)
    targets = jax.vmap(partial(slot_targets, experts=EXPERTS, capacity=CAP))(route_blocks)
    scaled = (mixing[:, :, None] * upstream[:, None, :].astype(jnp.float32)).astype(jnp.bfloat16)
    spread_tokens = jnp.repeat(tokens.reshape(sources, TOK_DEV, D), TOP, axis=1)
    spread_grads = scaled.reshape(sources, TOK_DEV * TOP, D)
    placing = jax.vmap(partial(place_rows, slot_count=slot_count))

    def to_experts(placed):
        return placed.reshape(sources, EXPERTS, CAP, D).transpose(1, 0, 2, 3).reshape(EXPERTS, sources * CAP, D)

    expert_tokens = to_experts(placing(targets, spread_tokens))
    expert_grads = to_experts(placing(targets, spread_grads))
    gate_whole = gate_matrix.reshape(EXPERTS, 2, D, FF_HALF).transpose(0, 2, 1, 3).reshape(EXPERTS, D, FF)
    up_whole = up_matrix.reshape(EXPERTS, 2, D, FF_HALF).transpose(0, 2, 1, 3).reshape(EXPERTS, D, FF)
    down_whole = down_matrix.reshape(EXPERTS, FF, D)

    def one_expert(inputs):
        token_rows, grad_rows, gate_mat, up_mat, down_mat = inputs
        gate_full, up_full, down_full, gate_grad, up_grad, scores = expert_backward(token_rows, grad_rows, gate_mat, up_mat, down_mat)
        blocks = 2 * N_TP
        block_width = FF // blocks

        def add_block(block_index, running):
            start = (block_index * block_width).astype(jnp.int32)
            gate_piece = lax.dynamic_slice_in_dim(gate_grad, start, block_width, 1)
            up_piece = lax.dynamic_slice_in_dim(up_grad, start, block_width, 1)
            gate_cols = lax.dynamic_slice_in_dim(gate_mat, start, block_width, 1)
            up_cols = lax.dynamic_slice_in_dim(up_mat, start, block_width, 1)
            contract_cols = (((1,), (1,)), ((), ()))
            block_term = lax.dot_general(gate_piece, gate_cols, contract_cols, preferred_element_type=jnp.float32)
            block_term = block_term + lax.dot_general(up_piece, up_cols, contract_cols, preferred_element_type=jnp.float32)
            rounded = lax.optimization_barrier(block_term.astype(jnp.bfloat16))
            return running + rounded.astype(jnp.float32)

        pair_grad = lax.fori_loop(0, blocks, add_block, jnp.zeros((token_rows.shape[0], D), jnp.float32))
        gate_norm = jnp.sum(jnp.square(gate_full).reshape(D, 2, FF_HALF), axis=2).T
        up_norm = jnp.sum(jnp.square(up_full).reshape(D, 2, FF_HALF), axis=2).T
        input_norm = jnp.stack([gate_norm, up_norm], axis=1)
        down_norm = jnp.sum(down_full * down_full, axis=1)
        return (gate_full.astype(jnp.bfloat16), up_full.astype(jnp.bfloat16), down_full.astype(jnp.bfloat16),
                input_norm, down_norm, pair_grad, scores)

    results = lax.map(one_expert, (expert_tokens, expert_grads, gate_whole, up_whole, down_whole))
    gate_out, up_out, down_out, input_norm, down_norm, pair_grad, scores = results
    gate_gradient = gate_out.reshape(EXPERTS, D, 2, FF_HALF).transpose(0, 2, 1, 3).reshape(SLABS, D, FF_HALF)
    up_gradient = up_out.reshape(EXPERTS, D, 2, FF_HALF).transpose(0, 2, 1, 3).reshape(SLABS, D, FF_HALF)
    down_gradient = down_out.reshape(SLABS, FF_HALF, D)
    input_norms = input_norm.reshape(SLABS, 2, D)
    down_norms = down_norm.reshape(SLABS, FF_HALF)
    back_rows = pair_grad.reshape(EXPERTS, sources, CAP, D).transpose(1, 0, 2, 3).reshape(sources, slot_count, D)
    gathered_rows = jax.vmap(take_rows)(back_rows, targets)
    token_gradient = jnp.sum(gathered_rows.reshape(TOKENS, TOP, D), axis=1).astype(jnp.bfloat16)
    back_scores = scores.reshape(EXPERTS, sources, CAP).transpose(1, 0, 2).reshape(sources, slot_count)
    mixing_gradient = jax.vmap(take_rows)(back_scores, targets).reshape(TOKENS, TOP) / mixing
    return (token_gradient, mixing_gradient, gate_gradient, up_gradient, down_gradient, input_norms, down_norms)
```

```python
import functools

import jax
import jax.numpy as jnp
from jax import lax
from jax.experimental import pallas as pl
from jax.experimental.pallas import tpu as pltpu
from jax.sharding import PartitionSpec as P

MESH = pl.DeviceIdType.MESH
F32 = jnp.float32
BF16 = jnp.bfloat16
NY = NX = 4
NT = NY * NX
NZ = 32
CAP = 10
GROUP = 8
NQ = NZ // GROUP
HALF = GROUP * CAP
ROWS = 2 * HALF
ALL = NQ * ROWS
SEND = 24
BACK = 16
LANES = 128


def offset_of(place):
    return (place + 1) // 2 if place % 2 else -(place // 2)


def opposite(place):
    if place in (0, NZ - 1):
        return place
    return place + 1 if place % 2 else place - 1


def dot(a, b, dims):
    return lax.dot_general(a, b, (dims, ((), ())), preferred_element_type=F32)


def iota(shape, dim):
    return lax.broadcasted_iota(jnp.int32, shape, dim)


def tenth(value):
    return ((value.astype(F32) + 0.5) * (1.0 / CAP)).astype(jnp.int32)


def body(
    tokens,
    upstream,
    routing,
    mixing,
    mixing_rows,
    gate_hbm,
    up_hbm,
    down_hbm,
    token_out,
    mixing_out,
    gate_out,
    up_out,
    down_out,
    norms_out,
    down_norms_out,
    w_in,
    w_down,
    z_send,
    z_recv,
    x_all,
    y_all,
    grads,
    hidden_all,
    part,
    part_in,
    part_sum,
    part_recv,
    score_own,
    score_in,
    score_sum,
    score_recv,
    back_send,
    back_recv,
    gate_full,
    up_full,
    down_full,
    norms,
    norms_recv,
    sem_w,
    sem_out,
    sem_send,
    sem_z,
    sem_first,
    sem_second,
    sem_core,
    sem_part,
    sem_score,
    sem_sum,
    sem_sum_score,
    sem_back,
    sem_norm,
):
    ep = lax.axis_index("ep")
    tp = lax.axis_index("tp")
    z, core = ep // 2, ep % 2
    y, x = tp // NX, tp % NX

    def at_z(offset):
        return (lax.rem(z + offset + NZ, NZ) * 2 + core, tp)

    def at_plane(dy, dx):
        return (ep, lax.rem(y + dy, NY) * NX + lax.rem(x + dx, NX))

    partner = (z * 2 + 1 - core, tp)
    plane = [(dy, dx) for dy in range(NY) for dx in range(NX) if (dy, dx) != (0, 0)]

    def send(source, target, stage, arrival, device):
        pltpu.make_async_remote_copy(
            src_ref=source,
            dst_ref=target,
            send_sem=sem_send.at[stage],
            recv_sem=arrival,
            device_id=device,
            device_id_type=MESH,
        ).start()

    def await_bytes(ref, sem):
        pltpu.make_async_copy(ref, ref, sem).wait()

    weights = [
        pltpu.make_async_copy(gate_hbm.at[0], w_in.at[:, pl.ds(0, LANES)], sem_w.at[0]),
        pltpu.make_async_copy(up_hbm.at[0], w_in.at[:, pl.ds(LANES, LANES)], sem_w.at[1]),
        pltpu.make_async_copy(down_hbm.at[0], w_down, sem_w.at[2]),
    ]
    for copy in weights:
        copy.start()

    barrier = pltpu.get_barrier_semaphore()
    for offset in range(1, NZ):
        pl.semaphore_signal(barrier, inc=1, device_id=at_z(offset), device_id_type=MESH)
    for dy, dx in plane:
        pl.semaphore_signal(barrier, inc=1, device_id=at_plane(dy, dx), device_id_type=MESH)
    pl.semaphore_signal(barrier, inc=1, device_id=partner, device_id_type=MESH)

    block = tokens.shape[0]
    upper = (iota((block, block), 0) < iota((block, block), 1)).astype(BF16)
    experts = iota((NZ, block), 0)
    chosen = [(routing[k : k + 1, :] == experts).astype(F32) for k in range(2)]
    earlier = [dot(c.astype(BF16), upper, ((1,), (0,))) for c in chosen]
    earlier[1] = earlier[1] + jnp.sum(chosen[0], axis=1, keepdims=True)
    places, slots = [], []
    for k in range(2):
        slots.append(jnp.sum(chosen[k] * earlier[k], axis=0, keepdims=True).astype(jnp.int32))
        ahead = routing[k : k + 1, :] - z
        ahead = jnp.where(ahead < 0, ahead + NZ, ahead)
        places.append(
            jnp.where(
                ahead == 0,
                0,
                jnp.where(ahead <= NZ // 2, 2 * ahead - 1, 2 * (NZ - ahead)),
            )
        )
    rows_out = iota((NZ * SEND, block), 0)
    token_hot, grad_hot = [], []
    for k in range(2):
        target = places[k] * SEND + slots[k]
        token_hot.append(rows_out == target)
        grad_hot.append((rows_out == target + CAP).astype(BF16))
    placed = dot((token_hot[0] | token_hot[1]).astype(BF16), tokens[...], ((1,), (0,)))
    cotangent = upstream[...].astype(F32)
    for k in range(2):
        scaled = (mixing[:, k : k + 1] * cotangent).astype(BF16)
        placed = placed + dot(grad_hot[k], scaled, ((1,), (0,)))
    z_send[...] = placed.reshape(NZ * SEND // 8, 8, LANES).astype(BF16)
    tiles = SEND // 8
    z_recv[0:tiles] = z_send[0:tiles]

    pl.semaphore_wait(barrier, NZ - 1 + len(plane) + 1)

    for place in range(1, NZ):
        send(
            z_send.at[pl.ds(place * tiles, tiles)],
            z_recv.at[pl.ds(opposite(place) * tiles, tiles)],
            0,
            sem_z.at[opposite(place) // GROUP],
            at_z(offset_of(place)),
        )

    row = iota((ROWS, GROUP * SEND), 0)
    col = iota((ROWS, GROUP * SEND), 1)
    low = row < HALF
    pair = jnp.where(low, row, row - HALF)
    source = tenth(pair)
    pick = (source * SEND + (pair - source * CAP) + jnp.where(low, 0, CAP) == col).astype(BF16)

    row = iota((GROUP * BACK, HALF), 0)
    col = iota((GROUP * BACK, HALF), 1)
    within = row % BACK
    spread = ((row // BACK * CAP + within == col) & (within < CAP)).astype(BF16)
    back_row = iota((GROUP * BACK, LANES), 0) % BACK

    for copy in weights:
        copy.wait()

    def own_rows(q):
        return pl.ds(pl.multiple_of(q * ROWS + core * HALF, 16), HALF)

    def other_rows(q):
        return pl.ds(pl.multiple_of(q * ROWS + (1 - core) * HALF, 16), HALF)

    def stage_gather_first(q):
        count = GROUP * tiles
        if q == 0:
            await_bytes(z_recv.at[pl.ds(tiles, count - tiles)], sem_z.at[0])
        else:
            await_bytes(z_recv.at[pl.ds(q * count, count)], sem_z.at[q])
        arrived = z_recv[pl.ds(q * count, count)].astype(F32).reshape(GROUP * SEND, LANES)
        rows = dot(pick, arrived.astype(BF16), ((1,), (0,))).astype(BF16)
        x_all[y, x, own_rows(q), :] = rows[:HALF]
        y_all[y, x, own_rows(q), :] = rows[HALF:]
        for d in range(1, NX):
            mine = x_all.at[y, x, own_rows(q), :]
            send(mine, mine, 1, sem_first.at[q, 0, d - 1], at_plane(0, d))
        for d in range(1, NY):
            mine = y_all.at[y, x, own_rows(q), :]
            send(mine, mine, 1, sem_first.at[q, 1, d - 1], at_plane(d, 0))

    def stage_gather_second(q):
        for d in range(1, NX):
            await_bytes(x_all.at[y, x, own_rows(q), :], sem_first.at[q, 0, d - 1])
        for d in range(1, NY):
            mine = x_all.at[y, :, own_rows(q), :]
            send(mine, mine, 2, sem_second.at[q, 0, d - 1], at_plane(d, 0))
        for d in range(1, NY):
            await_bytes(y_all.at[y, x, own_rows(q), :], sem_first.at[q, 1, d - 1])
        for d in range(1, NX):
            mine = y_all.at[:, x, own_rows(q), :]
            send(mine, mine, 2, sem_second.at[q, 1, d - 1], at_plane(0, d))

    def stage_cores(q):
        for d in range(1, NY):
            await_bytes(x_all.at[y, :, own_rows(q), :], sem_second.at[q, 0, d - 1])
        mine = x_all.at[:, :, own_rows(q), :]
        send(mine, mine, 3, sem_core.at[q, 0], partner)
        for d in range(1, NX):
            await_bytes(y_all.at[:, x, own_rows(q), :], sem_second.at[q, 1, d - 1])
        mine = y_all.at[:, :, own_rows(q), :]
        send(mine, mine, 3, sem_core.at[q, 1], partner)

    def stage_compute(q):
        rows = pl.ds(q * ROWS, ROWS)
        await_bytes(x_all.at[:, :, other_rows(q), :], sem_core.at[q, 0])
        x_rows = jnp.concatenate(
            [x_all[i, j, rows, :] for i in range(NY) for j in range(NX)], axis=1
        )
        pre = dot(x_rows, w_in[...], ((1,), (0,)))
        await_bytes(y_all.at[:, :, other_rows(q), :], sem_core.at[q, 1])
        y_rows = jnp.concatenate(
            [y_all[i, j, rows, :] for i in range(NY) for j in range(NX)], axis=1
        )
        back = dot(y_rows, w_down[...], ((1,), (1,)))
        gate_pre, up_pre = pre[:, :LANES], pre[:, LANES:]
        sig = jax.nn.sigmoid(gate_pre)
        act = gate_pre * sig
        hidden = act * up_pre
        gate_grad = (back * up_pre * sig * (1.0 + gate_pre * (1.0 - sig))).astype(BF16)
        up_grad = (back * act).astype(BF16)
        both = jnp.concatenate([gate_grad, up_grad], axis=1)
        grads[rows, :] = both
        hidden_all[rows, :] = hidden.astype(BF16)
        scores = jnp.sum(jnp.transpose(hidden * back), axis=0, keepdims=True)
        pad = jnp.zeros((1, LANES - HALF), F32)
        for half in range(2):
            score_own[q, half] = jnp.concatenate(
                [scores[:, half * HALF : (half + 1) * HALF], pad], axis=1
            )
        for b in range(NT // 2):
            term = dot(both, w_in[pl.ds(b * 2 * LANES, 2 * LANES), :], ((1,), (1,)))
            term = term.astype(BF16)
            for h in range(2):
                t = 2 * b + h
                part[t // NX, t % NX, rows, :] = term[:, h * LANES : (h + 1) * LANES]
        send(
            part.at[:, :, other_rows(q), :],
            part_in.at[q],
            4,
            sem_part.at[q],
            partner,
        )
        send(score_own.at[q, 1 - core], score_in.at[q], 5, sem_score.at[q], partner)

    def stage_pair_sum(q):
        await_bytes(part_in.at[q], sem_part.at[q])
        await_bytes(score_in.at[q], sem_score.at[q])
        total = part[:, :, own_rows(q), :].astype(F32) + part_in[q].astype(F32)
        part_sum[q] = total.astype(BF16)
        score_sum[q] = score_own[q, core] + score_in[q]
        for n, (dy, dx) in enumerate(plane):
            send(
                part_sum.at[q, lax.rem(y + dy, NY), lax.rem(x + dx, NX)],
                part_recv.at[q, n],
                6,
                sem_sum.at[q],
                at_plane(dy, dx),
            )
            send(score_sum.at[q], score_recv.at[q, n], 7, sem_sum_score.at[q], at_plane(dy, dx))

    def stage_back(q):
        await_bytes(part_recv.at[q], sem_sum.at[q])
        await_bytes(score_recv.at[q], sem_sum_score.at[q])
        total = part_sum[q, y, x].astype(F32)
        score = score_sum[q]
        for n in range(len(plane)):
            total = total + part_recv[q, n].astype(F32)
            score = score + score_recv[q, n]
        high = score.astype(BF16)
        rest = score - high.astype(F32)
        middle = rest.astype(BF16)
        low_bits = (rest - middle.astype(F32)).astype(BF16)
        message = dot(spread, total.astype(BF16), ((1,), (0,)))
        for n, piece in enumerate((high, middle, low_bits)):
            message = jnp.where(back_row == CAP + n, piece.astype(F32), message)
        message = message.astype(BF16)
        back_send[pl.ds(q * GROUP * BACK, GROUP * BACK), :] = message
        if q == 0:
            back_recv[0:BACK, :] = message[:BACK]
        for place in range(q * GROUP, (q + 1) * GROUP):
            if place:
                send(
                    back_send.at[pl.ds(place * BACK, BACK), :],
                    back_recv.at[pl.ds(opposite(place) * BACK, BACK), :],
                    8,
                    sem_back,
                    at_z(offset_of(place)),
                )

    def weight_in():
        def step(b, _):
            x_rows = x_all[b // NX, b % NX]
            full = dot(x_rows, grads[...], ((0,), (0,)))
            at = pl.ds(pl.multiple_of(b * LANES, LANES), LANES)
            gate_full[at, :] = full[:, :LANES].astype(BF16)
            up_full[at, :] = full[:, LANES:].astype(BF16)
            for h in range(2):
                piece = full[:, h * LANES : (h + 1) * LANES]
                norms[h : h + 1, at] = jnp.sum(
                    jnp.transpose(piece * piece), axis=0, keepdims=True
                )
            return 0

        lax.fori_loop(0, NT, step, 0)
        pltpu.make_async_copy(gate_full, gate_out.at[0], sem_out.at[0]).start()
        pltpu.make_async_copy(up_full, up_out.at[0], sem_out.at[1]).start()
        for n, (dy, dx) in enumerate(plane):
            send(norms, norms_recv.at[n], 9, sem_norm, at_plane(dy, dx))

    def weight_down():
        hidden_t = jnp.transpose(hidden_all[...].astype(F32)).astype(BF16)

        def step(b, squares):
            y_rows = jnp.concatenate(
                [y_all[b // 2, 2 * (b % 2)], y_all[b // 2, 2 * (b % 2) + 1]], axis=1
            )
            full = dot(hidden_t, y_rows, ((1,), (0,)))
            at = pl.ds(pl.multiple_of(b * 2 * LANES, 2 * LANES), 2 * LANES)
            down_full[:, at] = full.astype(BF16)
            left, right = full[:, :LANES], full[:, LANES:]
            return squares + left * left + right * right

        squares = lax.fori_loop(0, NT // 2, step, jnp.zeros((LANES, LANES), F32))
        down_norms_out[...] = jnp.sum(jnp.transpose(squares), axis=0, keepdims=True)
        pltpu.make_async_copy(down_full, down_out.at[0], sem_out.at[2]).start()

    stages = (
        (5, stage_back),
        (4, stage_pair_sum),
        (0, stage_gather_first),
        (1, stage_gather_second),
        (3, stage_compute),
        (2, stage_cores),
    )
    for step in range(NQ + 5):
        if step == NQ + 4:
            weight_in()
        for depth, stage in stages:
            if 0 <= step - depth < NQ:
                stage(step - depth)
    weight_down()

    await_bytes(back_recv.at[pl.ds(BACK, (NZ - 1) * BACK), :], sem_back)
    rows_back = iota((NZ * BACK, block), 0)
    returned = back_recv[...]
    row_hot = None
    for k in range(2):
        start = places[k] * BACK
        hot = rows_back == start + slots[k]
        row_hot = hot if row_hot is None else row_hot | hot
        score_hot = (rows_back >= start + CAP) & (rows_back < start + CAP + 3)
        mirrored = jnp.where(
            (places[k] == 0) | (places[k] == NZ - 1),
            places[k],
            jnp.where(places[k] % 2 == 1, places[k] + 1, places[k] - 1),
        )
        lane = mirrored % GROUP * CAP + slots[k]
        lines = dot(returned, score_hot.astype(BF16), ((0,), (0,)))
        score = jnp.sum(
            jnp.where(iota((LANES, block), 0) == lane, lines, 0.0), axis=0, keepdims=True
        )
        mixing_out[k : k + 1, :] = score / mixing_rows[k : k + 1, :]
    token_out[...] = dot(row_hot.astype(BF16), returned, ((0,), (0,))).astype(BF16)

    await_bytes(norms_recv, sem_norm)
    total = norms[...]
    for n in range(len(plane)):
        total = total + norms_recv[n]
    norms_out[0] = total

    for full, out, n in ((gate_full, gate_out, 0), (up_full, up_out, 1), (down_full, down_out, 2)):
        pltpu.make_async_copy(full, out.at[0], sem_out.at[n]).wait()
    sent = (
        z_recv.at[pl.ds(tiles, (NZ - 1) * tiles)],
        x_all.at[0, pl.ds(0, 3)],
        x_all.at[pl.ds(0, 3)],
        x_all,
        x_all.at[pl.ds(0, 2)],
        score_in,
        part_recv,
        score_recv,
        back_recv.at[pl.ds(BACK, (NZ - 1) * BACK), :],
        norms_recv,
    )
    for n, ref in enumerate(sent):
        await_bytes(ref, sem_send.at[n])


def on_device(tokens, routing, mixing, gate_matrix, up_matrix, down_matrix, upstream):
    vmem = pl.BlockSpec(memory_space=pltpu.VMEM)
    hbm = pl.BlockSpec(memory_space=pl.ANY)
    block = tokens.shape[0]
    shape = jax.ShapeDtypeStruct
    dma = pltpu.SemaphoreType.DMA
    results = pl.pallas_call(
        body,
        out_shape=(
            shape((block, LANES), BF16),
            shape((2, block), F32),
            shape(gate_matrix.shape, BF16),
            shape(up_matrix.shape, BF16),
            shape(down_matrix.shape, BF16),
            shape((1, 2, NT * LANES), F32),
            shape((1, LANES), F32),
        ),
        in_specs=[vmem] * 5 + [hbm] * 3,
        out_specs=(vmem, vmem, hbm, hbm, hbm, vmem, vmem),
        scratch_shapes=[
            pltpu.VMEM((NT * LANES, 2 * LANES), BF16),
            pltpu.VMEM((LANES, NT * LANES), BF16),
            pltpu.VMEM((NZ * SEND // 8, 8, LANES), BF16),
            pltpu.VMEM((NZ * SEND // 8, 8, LANES), BF16),
            pltpu.VMEM((NY, NX, ALL, LANES), BF16),
            pltpu.VMEM((NY, NX, ALL, LANES), BF16),
            pltpu.VMEM((ALL, 2 * LANES), BF16),
            pltpu.VMEM((ALL, LANES), BF16),
            pltpu.VMEM((NY, NX, ALL, LANES), BF16),
            pltpu.VMEM((NQ, NY, NX, HALF, LANES), BF16),
            pltpu.VMEM((NQ, NY, NX, HALF, LANES), BF16),
            pltpu.VMEM((NQ, NT - 1, HALF, LANES), BF16),
            pltpu.VMEM((NQ, 2, 1, LANES), F32),
            pltpu.VMEM((NQ, 1, LANES), F32),
            pltpu.VMEM((NQ, 1, LANES), F32),
            pltpu.VMEM((NQ, NT - 1, 1, LANES), F32),
            pltpu.VMEM((NZ * BACK, LANES), BF16),
            pltpu.VMEM((NZ * BACK, LANES), BF16),
            pltpu.VMEM((NT * LANES, LANES), BF16),
            pltpu.VMEM((NT * LANES, LANES), BF16),
            pltpu.VMEM((LANES, NT * LANES), BF16),
            pltpu.VMEM((2, NT * LANES), F32),
            pltpu.VMEM((NT - 1, 2, NT * LANES), F32),
            dma((3,)),
            dma((3,)),
            dma((10,)),
            dma((NQ,)),
            dma((NQ, 2, 3)),
            dma((NQ, 2, 3)),
            dma((NQ, 2)),
            dma((NQ,)),
            dma((NQ,)),
            dma((NQ,)),
            dma((NQ,)),
            dma,
            dma,
        ],
        compiler_params=pltpu.CompilerParams(
            collective_id=0, has_side_effects=True, vmem_limit_bytes=56 * 1024 * 1024
        ),
    )(
        tokens,
        upstream,
        routing.T,
        mixing,
        mixing.T,
        gate_matrix,
        up_matrix,
        down_matrix,
    )
    token_gradient, mixing_t, gate, up, down, norms, down_norms = results
    return token_gradient, mixing_t.T, gate, up, down, norms, down_norms


def solution(mesh):
    placed = (
        P("ep", "tp"),
        P("ep", None),
        P("ep", None),
        P("ep", None, "tp"),
        P("ep", None, "tp"),
        P("ep", "tp", None),
        P("ep", "tp"),
    )
    return jax.shard_map(
        on_device,
        mesh=mesh,
        in_specs=placed,
        out_specs=(
            P("ep", "tp"),
            P("ep", None),
            P("ep", None, "tp"),
            P("ep", None, "tp"),
            P("ep", "tp", None),
            P("ep", None, None),
            P("ep", "tp"),
        ),
        check_vma=False,
    )
```

```python
import functools

import jax
import jax.numpy as jnp
from jax import lax
from jax.experimental import pallas as pl
from jax.experimental.pallas import tpu as pltpu
from jax.sharding import PartitionSpec as P

MESH = pl.DeviceIdType.MESH
F32 = jnp.float32
BF16 = jnp.bfloat16
NY = NX = 4
NT = NY * NX
NZ = 32
CAP = 10
GROUP = 8
NQ = NZ // GROUP
HALF = GROUP * CAP
ROWS = 2 * HALF
ALL = NQ * ROWS
SEND = 24
BACK = 16
LANES = 128
ORDER = (
    ("A0", "B0", "R2", "R3", "A1", "C0", "B1", "D0", "A2", "C1", "E0", "B2", "D1")
    + ("A3", "C2", "E1", "B3", "D2", "F0", "C3", "E2", "F1", "D3", "E3", "F2")
)
REACH = NZ // 4
FAR = 2 * REACH + 1


def offset_of(place):
    return (place + 1) // 2 if place % 2 else -(place // 2)


def relay_of(place):
    return REACH if place % 2 else -REACH


def opposite(place):
    if place in (0, NZ - 1):
        return place
    return place + 1 if place % 2 else place - 1


def dot(a, b, dims):
    return lax.dot_general(a, b, (dims, ((), ())), preferred_element_type=F32)


def iota(shape, dim):
    return lax.broadcasted_iota(jnp.int32, shape, dim)


def tenth(value):
    return ((value.astype(F32) + 0.5) * (1.0 / CAP)).astype(jnp.int32)


def body(
    tokens_hbm,
    upstream_hbm,
    routing_hbm,
    mixing_hbm,
    gate_hbm,
    up_hbm,
    down_hbm,
    token_out,
    mixing_out,
    gate_full,
    up_full,
    down_full,
    norms_out,
    down_norms_out,
    tokens,
    upstream,
    routing,
    mixing_rows,
    w_in,
    w_down,
    z_send,
    z_recv,
    z_relay,
    x_all,
    y_all,
    grads,
    hidden_all,
    part,
    part_in,
    part_sum,
    part_recv,
    score_own,
    score_in,
    score_sum,
    score_recv,
    back_send,
    back_recv,
    norms,
    norms_recv,
    sem_in,
    sem_w,
    sem_send,
    sem_z,
    sem_relay,
    sem_first,
    sem_second,
    sem_core,
    sem_part,
    sem_score,
    sem_sum,
    sem_sum_score,
    sem_back,
    sem_norm,
):
    ep = lax.axis_index("ep")
    tp = lax.axis_index("tp")
    z, core = ep // 2, ep % 2
    y, x = tp // NX, tp % NX

    def at_z(offset):
        return (lax.rem(z + offset + NZ, NZ) * 2 + core, tp)

    def at_plane(dy, dx):
        return (ep, lax.rem(y + dy, NY) * NX + lax.rem(x + dx, NX))

    partner = (z * 2 + 1 - core, tp)
    plane = [(dy, dx) for dy in range(NY) for dx in range(NX) if (dy, dx) != (0, 0)]

    def send(source, target, stage, arrival, device):
        pltpu.make_async_remote_copy(
            src_ref=source,
            dst_ref=target,
            send_sem=sem_send.at[stage],
            recv_sem=arrival,
            device_id=device,
            device_id_type=MESH,
        ).start()

    def await_bytes(ref, sem):
        pltpu.make_async_copy(ref, ref, sem).wait()

    inputs = [
        pltpu.make_async_copy(source, target, sem_in.at[n])
        for n, (source, target) in enumerate(
            (
                (routing_hbm, routing),
                (mixing_hbm, mixing_rows),
                (tokens_hbm, tokens),
                (upstream_hbm, upstream),
            )
        )
    ]
    for copy in inputs:
        copy.start()
    weights = [
        pltpu.make_async_copy(gate_hbm.at[0], w_in.at[:, pl.ds(0, LANES)], sem_w.at[0]),
        pltpu.make_async_copy(up_hbm.at[0], w_in.at[:, pl.ds(LANES, LANES)], sem_w.at[1]),
        pltpu.make_async_copy(down_hbm.at[0], w_down, sem_w.at[2]),
    ]
    for copy in weights:
        copy.start()

    barrier = pltpu.get_barrier_semaphore()
    for place in range(1, FAR):
        pl.semaphore_signal(
            barrier, inc=1, device_id=at_z(offset_of(place)), device_id_type=MESH
        )
    for dy, dx in plane:
        pl.semaphore_signal(barrier, inc=1, device_id=at_plane(dy, dx), device_id_type=MESH)
    pl.semaphore_signal(barrier, inc=1, device_id=partner, device_id_type=MESH)

    for copy in inputs:
        copy.wait()

    block = tokens.shape[0]
    upper = (iota((block, block), 0) < iota((block, block), 1)).astype(BF16)
    experts = iota((NZ, block), 0)
    chosen = [(routing[k : k + 1, :] == experts).astype(F32) for k in range(2)]
    earlier = [dot(c.astype(BF16), upper, ((1,), (0,))) for c in chosen]
    earlier[1] = earlier[1] + jnp.sum(chosen[0], axis=1, keepdims=True)
    places, slots = [], []
    for k in range(2):
        slots.append(jnp.sum(chosen[k] * earlier[k], axis=0, keepdims=True).astype(jnp.int32))
        ahead = routing[k : k + 1, :] - z
        ahead = jnp.where(ahead < 0, ahead + NZ, ahead)
        places.append(
            jnp.where(
                ahead == 0,
                0,
                jnp.where(ahead <= NZ // 2, 2 * ahead - 1, 2 * (NZ - ahead)),
            )
        )
    rows_out = iota((NZ * SEND, block), 0)
    token_hot, grad_hot = [], []
    for k in range(2):
        target = places[k] * SEND + slots[k]
        token_hot.append(rows_out == target)
        grad_hot.append((rows_out == target + CAP).astype(BF16))
    placed = dot((token_hot[0] | token_hot[1]).astype(BF16), tokens[...], ((1,), (0,)))
    cotangent = upstream[...].astype(F32)
    for k in range(2):
        factor = jnp.transpose(jnp.broadcast_to(mixing_rows[k : k + 1, :], (LANES, block)))
        scaled = (factor * cotangent).astype(BF16)
        placed = placed + dot(grad_hot[k], scaled, ((1,), (0,)))
    z_send[...] = placed.reshape(NZ * SEND // 8, 8, LANES).astype(BF16)
    tiles = SEND // 8
    z_recv[0:tiles] = z_send[0:tiles]

    pl.semaphore_wait(barrier, FAR - 1 + len(plane) + 1)

    for place in range(FAR, NZ):
        send(
            z_send.at[pl.ds(place * tiles, tiles)],
            z_relay.at[pl.ds((place - FAR) * tiles, tiles)],
            0,
            sem_relay.at[place // GROUP - NQ // 2],
            at_z(relay_of(place)),
        )
    for place in range(1, FAR):
        send(
            z_send.at[pl.ds(place * tiles, tiles)],
            z_recv.at[pl.ds(opposite(place) * tiles, tiles)],
            0,
            sem_z.at[opposite(place) // GROUP],
            at_z(offset_of(place)),
        )

    row = iota((ROWS, GROUP * SEND), 0)
    col = iota((ROWS, GROUP * SEND), 1)
    low = row < HALF
    pair = jnp.where(low, row, row - HALF)
    source = tenth(pair)
    pick = (source * SEND + (pair - source * CAP) + jnp.where(low, 0, CAP) == col).astype(BF16)

    row = iota((GROUP * BACK, HALF), 0)
    col = iota((GROUP * BACK, HALF), 1)
    within = row % BACK
    spread = ((row // BACK * CAP + within == col) & (within < CAP)).astype(BF16)
    back_row = iota((GROUP * BACK, LANES), 0) % BACK

    for copy in weights:
        copy.wait()

    def own_rows(q):
        return pl.ds(pl.multiple_of(q * ROWS + core * HALF, 16), HALF)

    def other_rows(q):
        return pl.ds(pl.multiple_of(q * ROWS + (1 - core) * HALF, 16), HALF)

    def stage_relay(q):
        first = max(q * GROUP, FAR)
        last = (q + 1) * GROUP
        await_bytes(
            z_relay.at[pl.ds((first - FAR) * tiles, (last - first) * tiles)],
            sem_relay.at[q - NQ // 2],
        )
        for place in range(first, last):
            send(
                z_relay.at[pl.ds((place - FAR) * tiles, tiles)],
                z_recv.at[pl.ds(opposite(place) * tiles, tiles)],
                10,
                sem_z.at[opposite(place) // GROUP],
                at_z(offset_of(place) - relay_of(place)),
            )

    def stage_gather_first(q):
        count = GROUP * tiles
        if q == 0:
            await_bytes(z_recv.at[pl.ds(tiles, count - tiles)], sem_z.at[0])
        else:
            await_bytes(z_recv.at[pl.ds(q * count, count)], sem_z.at[q])
        arrived = z_recv[pl.ds(q * count, count)].astype(F32).reshape(GROUP * SEND, LANES)
        rows = dot(pick, arrived.astype(BF16), ((1,), (0,))).astype(BF16)
        x_all[y, x, own_rows(q), :] = rows[:HALF]
        y_all[y, x, own_rows(q), :] = rows[HALF:]
        for d in range(1, NX):
            mine = x_all.at[y, x, own_rows(q), :]
            send(mine, mine, 1, sem_first.at[q, 0, d - 1], at_plane(0, d))
        for d in range(1, NY):
            mine = y_all.at[y, x, own_rows(q), :]
            send(mine, mine, 1, sem_first.at[q, 1, d - 1], at_plane(d, 0))

    def stage_gather_second(q):
        for d in range(1, NX):
            await_bytes(x_all.at[y, x, own_rows(q), :], sem_first.at[q, 0, d - 1])
        for d in range(1, NY):
            mine = x_all.at[y, :, own_rows(q), :]
            send(mine, mine, 2, sem_second.at[q, 0, d - 1], at_plane(d, 0))
        for d in range(1, NY):
            await_bytes(y_all.at[y, x, own_rows(q), :], sem_first.at[q, 1, d - 1])
        for d in range(1, NX):
            mine = y_all.at[:, x, own_rows(q), :]
            send(mine, mine, 2, sem_second.at[q, 1, d - 1], at_plane(0, d))

    def stage_cores(q):
        for d in range(1, NY):
            await_bytes(x_all.at[y, :, own_rows(q), :], sem_second.at[q, 0, d - 1])
        mine = x_all.at[:, :, own_rows(q), :]
        send(mine, mine, 3, sem_core.at[q, 0], partner)
        for d in range(1, NX):
            await_bytes(y_all.at[:, x, own_rows(q), :], sem_second.at[q, 1, d - 1])
        mine = y_all.at[:, :, own_rows(q), :]
        send(mine, mine, 3, sem_core.at[q, 1], partner)

    def stage_compute(q):
        rows = pl.ds(q * ROWS, ROWS)
        await_bytes(x_all.at[:, :, other_rows(q), :], sem_core.at[q, 0])
        x_rows = jnp.concatenate(
            [x_all[i, j, rows, :] for i in range(NY) for j in range(NX)], axis=1
        )
        pre = dot(x_rows, w_in[...], ((1,), (0,)))
        await_bytes(y_all.at[:, :, other_rows(q), :], sem_core.at[q, 1])
        y_rows = jnp.concatenate(
            [y_all[i, j, rows, :] for i in range(NY) for j in range(NX)], axis=1
        )
        back = dot(y_rows, w_down[...], ((1,), (1,)))
        gate_pre, up_pre = pre[:, :LANES], pre[:, LANES:]
        sig = jax.nn.sigmoid(gate_pre)
        act = gate_pre * sig
        hidden = act * up_pre
        gate_grad = (back * up_pre * sig * (1.0 + gate_pre * (1.0 - sig))).astype(BF16)
        up_grad = (back * act).astype(BF16)
        both = jnp.concatenate([gate_grad, up_grad], axis=1)
        grads[rows, :] = both
        hidden_all[rows, :] = hidden.astype(BF16)
        scores = jnp.sum(jnp.transpose(hidden * back), axis=0, keepdims=True)
        pad = jnp.zeros((1, LANES - HALF), F32)
        for half in range(2):
            score_own[q, half] = jnp.concatenate(
                [scores[:, half * HALF : (half + 1) * HALF], pad], axis=1
            )
        for b in range(NT // 2):
            term = dot(both, w_in[pl.ds(b * 2 * LANES, 2 * LANES), :], ((1,), (1,)))
            term = term.astype(BF16)
            for h in range(2):
                t = 2 * b + h
                part[t // NX, t % NX, rows, :] = term[:, h * LANES : (h + 1) * LANES]
        send(
            part.at[:, :, other_rows(q), :],
            part_in.at[q],
            4,
            sem_part.at[q],
            partner,
        )
        send(score_own.at[q, 1 - core], score_in.at[q], 5, sem_score.at[q], partner)

    def stage_pair_sum(q):
        await_bytes(part_in.at[q], sem_part.at[q])
        await_bytes(score_in.at[q], sem_score.at[q])
        total = part[:, :, own_rows(q), :].astype(F32) + part_in[q].astype(F32)
        part_sum[q] = total.astype(BF16)
        score_sum[q] = score_own[q, core] + score_in[q]
        for n, (dy, dx) in enumerate(plane):
            send(
                part_sum.at[q, lax.rem(y + dy, NY), lax.rem(x + dx, NX)],
                part_recv.at[q, n],
                6,
                sem_sum.at[q],
                at_plane(dy, dx),
            )
            send(score_sum.at[q], score_recv.at[q, n], 7, sem_sum_score.at[q], at_plane(dy, dx))

    def stage_back(q):
        await_bytes(part_recv.at[q], sem_sum.at[q])
        await_bytes(score_recv.at[q], sem_sum_score.at[q])
        total = part_sum[q, y, x].astype(F32)
        score = score_sum[q]
        for n in range(len(plane)):
            total = total + part_recv[q, n].astype(F32)
            score = score + score_recv[q, n]
        high = score.astype(BF16)
        rest = score - high.astype(F32)
        middle = rest.astype(BF16)
        low_bits = (rest - middle.astype(F32)).astype(BF16)
        message = dot(spread, total.astype(BF16), ((1,), (0,)))
        for n, piece in enumerate((high, middle, low_bits)):
            message = jnp.where(back_row == CAP + n, piece.astype(F32), message)
        message = message.astype(BF16)
        back_send[pl.ds(q * GROUP * BACK, GROUP * BACK), :] = message
        if q == 0:
            back_recv[0:BACK, :] = message[:BACK]
        for place in range(q * GROUP, (q + 1) * GROUP):
            if place:
                send(
                    back_send.at[pl.ds(place * BACK, BACK), :],
                    back_recv.at[pl.ds(opposite(place) * BACK, BACK), :],
                    8,
                    sem_back,
                    at_z(offset_of(place)),
                )

    def weight_in(begin, end):
        def step(b, _):
            x_rows = x_all[b // NX, b % NX]
            full = dot(x_rows, grads[...], ((0,), (0,)))
            at = pl.ds(pl.multiple_of(b * LANES, LANES), LANES)
            gate_full[0, at, :] = full[:, :LANES].astype(BF16)
            up_full[0, at, :] = full[:, LANES:].astype(BF16)
            for h in range(2):
                piece = full[:, h * LANES : (h + 1) * LANES]
                norms[h : h + 1, at] = jnp.sum(
                    jnp.transpose(piece * piece), axis=0, keepdims=True
                )
            return 0

        lax.fori_loop(begin, end, step, 0)
        if end == NT:
            for n, (dy, dx) in enumerate(plane):
                send(norms, norms_recv.at[n], 9, sem_norm, at_plane(dy, dx))

    def weight_down():
        hidden_t = jnp.transpose(hidden_all[...].astype(F32)).astype(BF16)

        def step(b, squares):
            y_rows = jnp.concatenate(
                [y_all[b // 2, 2 * (b % 2)], y_all[b // 2, 2 * (b % 2) + 1]], axis=1
            )
            full = dot(hidden_t, y_rows, ((1,), (0,)))
            at = pl.ds(pl.multiple_of(b * 2 * LANES, 2 * LANES), 2 * LANES)
            down_full[0, :, at] = full.astype(BF16)
            left, right = full[:, :LANES], full[:, LANES:]
            return squares + left * left + right * right

        squares = lax.fori_loop(0, NT // 2, step, jnp.zeros((LANES, LANES), F32))
        down_norms_out[...] = jnp.sum(jnp.transpose(squares), axis=0, keepdims=True)

    stages = dict(
        A=stage_gather_first,
        B=stage_gather_second,
        C=stage_cores,
        D=stage_compute,
        E=stage_pair_sum,
        F=stage_back,
        R=stage_relay,
    )
    for name, q in ORDER:
        stages[name](int(q))
    weight_down()
    weight_in(0, NT // 2)
    stage_back(NQ - 1)
    weight_in(NT // 2, NT)

    await_bytes(back_recv.at[pl.ds(BACK, (NZ - 1) * BACK), :], sem_back)
    rows_back = iota((NZ * BACK, block), 0)
    returned = back_recv[...]
    row_hot = None
    for k in range(2):
        start = places[k] * BACK
        hot = rows_back == start + slots[k]
        row_hot = hot if row_hot is None else row_hot | hot
        score_hot = (rows_back >= start + CAP) & (rows_back < start + CAP + 3)
        mirrored = jnp.where(
            (places[k] == 0) | (places[k] == NZ - 1),
            places[k],
            jnp.where(places[k] % 2 == 1, places[k] + 1, places[k] - 1),
        )
        lane = mirrored % GROUP * CAP + slots[k]
        lines = dot(returned, score_hot.astype(BF16), ((0,), (0,)))
        score = jnp.sum(
            jnp.where(iota((LANES, block), 0) == lane, lines, 0.0), axis=0, keepdims=True
        )
        mixing_out[k : k + 1, :] = score / mixing_rows[k : k + 1, :]
    token_out[...] = dot(row_hot.astype(BF16), returned, ((0,), (0,))).astype(BF16)

    await_bytes(norms_recv, sem_norm)
    total = norms[...]
    for n in range(len(plane)):
        total = total + norms_recv[n]
    norms_out[0] = total

    sent = (
        z_recv.at[pl.ds(tiles, (NZ - 1) * tiles)],
        x_all.at[0, pl.ds(0, 3)],
        x_all.at[pl.ds(0, 3)],
        x_all,
        x_all.at[pl.ds(0, 2)],
        score_in,
        part_recv,
        score_recv,
        back_recv.at[pl.ds(BACK, (NZ - 1) * BACK), :],
        norms_recv,
        z_relay,
    )
    for n, ref in enumerate(sent):
        await_bytes(ref, sem_send.at[n])


def write_out(*refs):
    count = len(refs) // 2
    sems = refs[-1]
    copies = [
        pltpu.make_async_copy(refs[n], refs[count + n], sems.at[n]) for n in range(count)
    ]
    for copy in copies:
        copy.start()
    for copy in copies:
        copy.wait()


def on_device(tokens, routing, mixing, gate_matrix, up_matrix, down_matrix, upstream):
    vmem = pl.BlockSpec(memory_space=pltpu.VMEM)
    hbm = pl.BlockSpec(memory_space=pltpu.HBM)
    block = tokens.shape[0]
    shape = jax.ShapeDtypeStruct
    dma = pltpu.SemaphoreType.DMA
    shapes = (
        shape((block, LANES), BF16),
        shape((2, block), F32),
        shape(gate_matrix.shape, BF16),
        shape(up_matrix.shape, BF16),
        shape(down_matrix.shape, BF16),
        shape((1, 2, NT * LANES), F32),
        shape((1, LANES), F32),
    )
    results = pl.pallas_call(
        body,
        out_shape=tuple(pltpu.VMEM(s.shape, s.dtype) for s in shapes),
        in_specs=[hbm] * 7,
        out_specs=[vmem] * 7,
        scratch_shapes=[
            pltpu.VMEM((block, LANES), BF16),
            pltpu.VMEM((block, LANES), BF16),
            pltpu.VMEM((2, block), jnp.int32),
            pltpu.VMEM((2, block), F32),
            pltpu.VMEM((NT * LANES, 2 * LANES), BF16),
            pltpu.VMEM((LANES, NT * LANES), BF16),
            pltpu.VMEM((NZ * SEND // 8, 8, LANES), BF16),
            pltpu.VMEM((NZ * SEND // 8, 8, LANES), BF16),
            pltpu.VMEM(((NZ - FAR) * SEND // 8, 8, LANES), BF16),
            pltpu.VMEM((NY, NX, ALL, LANES), BF16),
            pltpu.VMEM((NY, NX, ALL, LANES), BF16),
            pltpu.VMEM((ALL, 2 * LANES), BF16),
            pltpu.VMEM((ALL, LANES), BF16),
            pltpu.VMEM((NY, NX, ALL, LANES), BF16),
            pltpu.VMEM((NQ, NY, NX, HALF, LANES), BF16),
            pltpu.VMEM((NQ, NY, NX, HALF, LANES), BF16),
            pltpu.VMEM((NQ, NT - 1, HALF, LANES), BF16),
            pltpu.VMEM((NQ, 2, 1, LANES), F32),
            pltpu.VMEM((NQ, 1, LANES), F32),
            pltpu.VMEM((NQ, 1, LANES), F32),
            pltpu.VMEM((NQ, NT - 1, 1, LANES), F32),
            pltpu.VMEM((NZ * BACK, LANES), BF16),
            pltpu.VMEM((NZ * BACK, LANES), BF16),
            pltpu.VMEM((2, NT * LANES), F32),
            pltpu.VMEM((NT - 1, 2, NT * LANES), F32),
            dma((4,)),
            dma((3,)),
            dma((11,)),
            dma((NQ,)),
            dma((NQ // 2,)),
            dma((NQ, 2, 3)),
            dma((NQ, 2, 3)),
            dma((NQ, 2)),
            dma((NQ,)),
            dma((NQ,)),
            dma((NQ,)),
            dma((NQ,)),
            dma,
            dma,
        ],
        compiler_params=pltpu.CompilerParams(
            collective_id=0, has_side_effects=True, vmem_limit_bytes=56 * 1024 * 1024
        ),
    )(
        tokens,
        upstream,
        routing.T,
        mixing.T,
        gate_matrix,
        up_matrix,
        down_matrix,
    )
    results = pl.pallas_call(
        write_out,
        out_shape=shapes,
        in_specs=[vmem] * 7,
        out_specs=[hbm] * 7,
        scratch_shapes=[dma((7,))],
    )(*(pltpu.with_memory_space_constraint(r, pltpu.VMEM) for r in results))
    token_gradient, mixing_t, gate, up, down, norms, down_norms = results
    return token_gradient, mixing_t.T, gate, up, down, norms, down_norms


def solution(mesh):
    placed = (
        P("ep", "tp"),
        P("ep", None),
        P("ep", None),
        P("ep", None, "tp"),
        P("ep", None, "tp"),
        P("ep", "tp", None),
        P("ep", "tp"),
    )
    return jax.shard_map(
        on_device,
        mesh=mesh,
        in_specs=placed,
        out_specs=(
            P("ep", "tp"),
            P("ep", None),
            P("ep", None, "tp"),
            P("ep", None, "tp"),
            P("ep", "tp", None),
            P("ep", None, None),
            P("ep", "tp"),
        ),
        check_vma=False,
    )
```

```python
import functools

import jax
import jax.numpy as jnp
from jax import lax
from jax.experimental import pallas as pl
from jax.experimental.pallas import tpu as pltpu
from jax.sharding import PartitionSpec as P

MESH = pl.DeviceIdType.MESH
F32 = jnp.float32
BF16 = jnp.bfloat16
NY = NX = 4
NT = NY * NX
NZ = 32
CAP = 10
GROUP = 8
NQ = NZ // GROUP
HALF = GROUP * CAP
ROWS = 2 * HALF
ALL = NQ * ROWS
SEND = 24
BACK = 16
LANES = 128
ORDER = (
    ("A0", "B0", "R2", "R3", "G0", "A1", "C0", "A2", "A3", "B1", "D0", "B2", "E0", "B3", "G1")
    + ("G2", "C1", "G3", "C2", "C3", "D1", "H0", "D2", "E1", "F0", "D3", "E2", "E3", "H1")
)
SPLIT = 48
REACH = NZ // 4
FAR = 2 * REACH + 1


def offset_of(place):
    return (place + 1) // 2 if place % 2 else -(place // 2)


def relay_of(place):
    return REACH if place % 2 else -REACH


def opposite(place):
    if place in (0, NZ - 1):
        return place
    return place + 1 if place % 2 else place - 1


def dot(a, b, dims):
    return lax.dot_general(a, b, (dims, ((), ())), preferred_element_type=F32)


def iota(shape, dim):
    return lax.broadcasted_iota(jnp.int32, shape, dim)


def tenth(value):
    return ((value.astype(F32) + 0.5) * (1.0 / CAP)).astype(jnp.int32)


def body(
    tokens_hbm,
    upstream_hbm,
    routing_hbm,
    mixing_hbm,
    gate_hbm,
    up_hbm,
    down_hbm,
    token_out,
    mixing_out,
    gate_full,
    up_full,
    down_full,
    norms_out,
    down_norms_out,
    tokens,
    upstream,
    routing,
    mixing_rows,
    w_in,
    w_down,
    z_send,
    z_recv,
    z_relay,
    x_all,
    y_all,
    grads,
    hidden_all,
    part,
    part_in,
    part_sum,
    row_recv,
    col_recv,
    row_sum,
    col_sum,
    row_last,
    col_last,
    score_own,
    score_in,
    score_sum,
    score_recv,
    back_send,
    back_recv,
    norms,
    norms_recv,
    sem_in,
    sem_w,
    sem_send,
    sem_z,
    sem_relay,
    sem_first,
    sem_second,
    sem_forward,
    sem_core,
    sem_part,
    sem_score,
    sem_row,
    sem_col,
    sem_row_last,
    sem_col_last,
    sem_sum_score,
    sem_back,
    sem_norm,
):
    ep = lax.axis_index("ep")
    tp = lax.axis_index("tp")
    z, core = ep // 2, ep % 2
    y, x = tp // NX, tp % NX

    def at_z(offset):
        return (lax.rem(z + offset + NZ, NZ) * 2 + core, tp)

    def at_plane(dy, dx):
        return (ep, lax.rem(y + dy, NY) * NX + lax.rem(x + dx, NX))

    partner = (z * 2 + 1 - core, tp)
    plane = [(dy, dx) for dy in range(NY) for dx in range(NX) if (dy, dx) != (0, 0)]

    def send(source, target, stage, arrival, device):
        pltpu.make_async_remote_copy(
            src_ref=source,
            dst_ref=target,
            send_sem=sem_send.at[stage],
            recv_sem=arrival,
            device_id=device,
            device_id_type=MESH,
        ).start()

    def await_bytes(ref, sem):
        pltpu.make_async_copy(ref, ref, sem).wait()

    inputs = [
        pltpu.make_async_copy(source, target, sem_in.at[n])
        for n, (source, target) in enumerate(
            (
                (routing_hbm, routing),
                (mixing_hbm, mixing_rows),
                (tokens_hbm, tokens),
                (upstream_hbm, upstream),
            )
        )
    ]
    for copy in inputs:
        copy.start()
    weights = [
        pltpu.make_async_copy(gate_hbm.at[0], w_in.at[:, pl.ds(0, LANES)], sem_w.at[0]),
        pltpu.make_async_copy(up_hbm.at[0], w_in.at[:, pl.ds(LANES, LANES)], sem_w.at[1]),
        pltpu.make_async_copy(down_hbm.at[0], w_down, sem_w.at[2]),
    ]
    for copy in weights:
        copy.start()

    barrier = pltpu.get_barrier_semaphore()
    for place in range(1, FAR):
        pl.semaphore_signal(
            barrier, inc=1, device_id=at_z(offset_of(place)), device_id_type=MESH
        )
    for dy, dx in plane:
        pl.semaphore_signal(barrier, inc=1, device_id=at_plane(dy, dx), device_id_type=MESH)
    pl.semaphore_signal(barrier, inc=1, device_id=partner, device_id_type=MESH)

    for copy in inputs:
        copy.wait()

    block = tokens.shape[0]
    upper = (iota((block, block), 0) < iota((block, block), 1)).astype(BF16)
    experts = iota((NZ, block), 0)
    chosen = [(routing[k : k + 1, :] == experts).astype(F32) for k in range(2)]
    earlier = [dot(c.astype(BF16), upper, ((1,), (0,))) for c in chosen]
    earlier[1] = earlier[1] + jnp.sum(chosen[0], axis=1, keepdims=True)
    places, slots = [], []
    for k in range(2):
        slots.append(jnp.sum(chosen[k] * earlier[k], axis=0, keepdims=True).astype(jnp.int32))
        ahead = routing[k : k + 1, :] - z
        ahead = jnp.where(ahead < 0, ahead + NZ, ahead)
        places.append(
            jnp.where(
                ahead == 0,
                0,
                jnp.where(ahead <= NZ // 2, 2 * ahead - 1, 2 * (NZ - ahead)),
            )
        )
    rows_out = iota((NZ * SEND, block), 0)
    token_hot, grad_hot = [], []
    for k in range(2):
        target = places[k] * SEND + slots[k]
        token_hot.append(rows_out == target)
        grad_hot.append((rows_out == target + CAP).astype(BF16))
    placed = dot((token_hot[0] | token_hot[1]).astype(BF16), tokens[...], ((1,), (0,)))
    cotangent = upstream[...].astype(F32)
    for k in range(2):
        factor = jnp.transpose(jnp.broadcast_to(mixing_rows[k : k + 1, :], (LANES, block)))
        scaled = (factor * cotangent).astype(BF16)
        placed = placed + dot(grad_hot[k], scaled, ((1,), (0,)))
    z_send[...] = placed.reshape(NZ * SEND // 8, 8, LANES).astype(BF16)
    tiles = SEND // 8
    z_recv[0:tiles] = z_send[0:tiles]

    pl.semaphore_wait(barrier, FAR - 1 + len(plane) + 1)

    for place in range(1, GROUP + 1):
        send(
            z_send.at[pl.ds(place * tiles, tiles)],
            z_recv.at[pl.ds(opposite(place) * tiles, tiles)],
            0,
            sem_z.at[opposite(place) // GROUP],
            at_z(offset_of(place)),
        )
    for place in range(FAR, NZ):
        send(
            z_send.at[pl.ds(place * tiles, tiles)],
            z_relay.at[pl.ds((place - FAR) * tiles, tiles)],
            0,
            sem_relay.at[place // GROUP - NQ // 2],
            at_z(relay_of(place)),
        )
    for place in range(GROUP + 1, FAR):
        send(
            z_send.at[pl.ds(place * tiles, tiles)],
            z_recv.at[pl.ds(opposite(place) * tiles, tiles)],
            0,
            sem_z.at[opposite(place) // GROUP],
            at_z(offset_of(place)),
        )

    row = iota((ROWS, GROUP * SEND), 0)
    col = iota((ROWS, GROUP * SEND), 1)
    low = row < HALF
    pair = jnp.where(low, row, row - HALF)
    source = tenth(pair)
    pick = (source * SEND + (pair - source * CAP) + jnp.where(low, 0, CAP) == col).astype(BF16)

    row = iota((GROUP * BACK, HALF), 0)
    col = iota((GROUP * BACK, HALF), 1)
    within = row % BACK
    spread = ((row // BACK * CAP + within == col) & (within < CAP)).astype(BF16)
    back_row = iota((GROUP * BACK, LANES), 0) % BACK

    for copy in weights:
        copy.wait()

    def own_rows(q):
        return pl.ds(pl.multiple_of(q * ROWS + core * HALF, 16), HALF)

    def other_rows(q):
        return pl.ds(pl.multiple_of(q * ROWS + (1 - core) * HALF, 16), HALF)

    def stage_relay(q):
        first = max(q * GROUP, FAR)
        last = (q + 1) * GROUP
        await_bytes(
            z_relay.at[pl.ds((first - FAR) * tiles, (last - first) * tiles)],
            sem_relay.at[q - NQ // 2],
        )
        for place in range(first, last):
            send(
                z_relay.at[pl.ds((place - FAR) * tiles, tiles)],
                z_recv.at[pl.ds(opposite(place) * tiles, tiles)],
                10,
                sem_z.at[opposite(place) // GROUP],
                at_z(offset_of(place) - relay_of(place)),
            )

    def stage_gather_first(q):
        count = GROUP * tiles
        if q == 0:
            await_bytes(z_recv.at[pl.ds(tiles, count - tiles)], sem_z.at[0])
        else:
            await_bytes(z_recv.at[pl.ds(q * count, count)], sem_z.at[q])
        arrived = z_recv[pl.ds(q * count, count)].astype(F32).reshape(GROUP * SEND, LANES)
        rows = dot(pick, arrived.astype(BF16), ((1,), (0,))).astype(BF16)
        x_all[y, x, own_rows(q), :] = rows[:HALF]
        y_all[y, x, own_rows(q), :] = rows[HALF:]
        for d in range(1, NX):
            mine = x_all.at[y, x, own_rows(q), :]
            send(mine, mine, 1, sem_first.at[q, 0, d - 1], at_plane(0, d))
        for d in range(1, NY):
            mine = y_all.at[y, x, own_rows(q), :]
            send(mine, mine, 1, sem_first.at[q, 1, d - 1], at_plane(d, 0))

    def stage_gather_second(q):
        for d in range(1, NX):
            await_bytes(x_all.at[y, x, own_rows(q), :], sem_first.at[q, 0, d - 1])
        for d in (1, NY - 1):
            mine = x_all.at[y, :, own_rows(q), :]
            send(mine, mine, 2, sem_second.at[q, 0, d // 2], at_plane(d, 0))
        for d in range(1, NY):
            await_bytes(y_all.at[y, x, own_rows(q), :], sem_first.at[q, 1, d - 1])
        for d in (1, NX - 1):
            mine = y_all.at[:, x, own_rows(q), :]
            send(mine, mine, 2, sem_second.at[q, 1, d // 2], at_plane(0, d))

    def stage_forward(q):
        for n, d in enumerate((1, NY - 1)):
            await_bytes(x_all.at[y, :, own_rows(q), :], sem_second.at[q, 0, n])
            theirs = x_all.at[lax.rem(y + NY - d, NY), pl.ds(2 * n, 2), own_rows(q), :]
            send(theirs, theirs, 11, sem_forward.at[q, 0, n], at_plane(d, 0))
        for n, d in enumerate((1, NX - 1)):
            await_bytes(y_all.at[:, x, own_rows(q), :], sem_second.at[q, 1, n])
            theirs = y_all.at[pl.ds(2 * n, 2), lax.rem(x + NX - d, NX), own_rows(q), :]
            send(theirs, theirs, 11, sem_forward.at[q, 1, n], at_plane(0, d))

    def stage_cores(q):
        for n in range(2):
            await_bytes(x_all.at[y, pl.ds(0, 2), own_rows(q), :], sem_forward.at[q, 0, n])
        mine = x_all.at[:, :, own_rows(q), :]
        send(mine, mine, 3, sem_core.at[q, 0], partner)
        for n in range(2):
            await_bytes(y_all.at[pl.ds(0, 2), x, own_rows(q), :], sem_forward.at[q, 1, n])
        mine = y_all.at[:, :, own_rows(q), :]
        send(mine, mine, 3, sem_core.at[q, 1], partner)

    def stage_compute(q):
        rows = pl.ds(q * ROWS, ROWS)
        await_bytes(x_all.at[:, :, other_rows(q), :], sem_core.at[q, 0])
        x_rows = jnp.concatenate(
            [x_all[i, j, rows, :] for i in range(NY) for j in range(NX)], axis=1
        )
        pre = dot(x_rows, w_in[...], ((1,), (0,)))
        await_bytes(y_all.at[:, :, other_rows(q), :], sem_core.at[q, 1])
        y_rows = jnp.concatenate(
            [y_all[i, j, rows, :] for i in range(NY) for j in range(NX)], axis=1
        )
        back = dot(y_rows, w_down[...], ((1,), (1,)))
        gate_pre, up_pre = pre[:, :LANES], pre[:, LANES:]
        sig = jax.nn.sigmoid(gate_pre)
        act = gate_pre * sig
        hidden = act * up_pre
        gate_grad = (back * up_pre * sig * (1.0 + gate_pre * (1.0 - sig))).astype(BF16)
        up_grad = (back * act).astype(BF16)
        both = jnp.concatenate([gate_grad, up_grad], axis=1)
        grads[rows, :] = both
        hidden_all[rows, :] = hidden.astype(BF16)
        scores = jnp.sum(jnp.transpose(hidden * back), axis=0, keepdims=True)
        pad = jnp.zeros((1, LANES - HALF), F32)
        for half in range(2):
            score_own[q, half] = jnp.concatenate(
                [scores[:, half * HALF : (half + 1) * HALF], pad], axis=1
            )
        for b in range(NT // 2):
            term = dot(both, w_in[pl.ds(b * 2 * LANES, 2 * LANES), :], ((1,), (1,)))
            term = term.astype(BF16)
            for h in range(2):
                t = 2 * b + h
                part[t // NX, t % NX, rows, :] = term[:, h * LANES : (h + 1) * LANES]
        send(
            part.at[:, :, other_rows(q), :],
            part_in.at[q],
            4,
            sem_part.at[q],
            partner,
        )
        send(score_own.at[q, 1 - core], score_in.at[q], 5, sem_score.at[q], partner)

    def stage_pair_sum(q):
        await_bytes(part_in.at[q], sem_part.at[q])
        await_bytes(score_in.at[q], sem_score.at[q])
        total = part[:, :, own_rows(q), :].astype(F32) + part_in[q].astype(F32)
        part_sum[q] = total.astype(BF16)
        score_sum[q] = score_own[q, core] + score_in[q]
        for d in range(1, NX):
            send(
                part_sum.at[q, :, lax.rem(x + d, NX), pl.ds(0, SPLIT), :],
                row_recv.at[q, d - 1],
                6,
                sem_row.at[q],
                at_plane(0, d),
            )
        for d in range(1, NY):
            send(
                part_sum.at[q, lax.rem(y + d, NY), :, pl.ds(SPLIT, HALF - SPLIT), :],
                col_recv.at[q, d - 1],
                12,
                sem_col.at[q],
                at_plane(d, 0),
            )
        for n, (dy, dx) in enumerate(plane):
            send(score_sum.at[q], score_recv.at[q, n], 7, sem_sum_score.at[q], at_plane(dy, dx))

    def stage_reduce(q):
        await_bytes(row_recv.at[q], sem_row.at[q])
        total = part_sum[q, :, x, pl.ds(0, SPLIT), :].astype(F32)
        for n in range(NX - 1):
            total = total + row_recv[q, n].astype(F32)
        row_sum[q] = total.astype(BF16)
        for d in range(1, NY):
            send(
                row_sum.at[q, lax.rem(y + d, NY)],
                row_last.at[q, d - 1],
                13,
                sem_row_last.at[q],
                at_plane(d, 0),
            )
        await_bytes(col_recv.at[q], sem_col.at[q])
        total = part_sum[q, y, :, pl.ds(SPLIT, HALF - SPLIT), :].astype(F32)
        for n in range(NY - 1):
            total = total + col_recv[q, n].astype(F32)
        col_sum[q] = total.astype(BF16)
        for d in range(1, NX):
            send(
                col_sum.at[q, lax.rem(x + d, NX)],
                col_last.at[q, d - 1],
                14,
                sem_col_last.at[q],
                at_plane(0, d),
            )

    def stage_back(q):
        await_bytes(row_last.at[q], sem_row_last.at[q])
        await_bytes(col_last.at[q], sem_col_last.at[q])
        await_bytes(score_recv.at[q], sem_sum_score.at[q])
        rows = row_sum[q, y].astype(F32)
        for n in range(NY - 1):
            rows = rows + row_last[q, n].astype(F32)
        cols = col_sum[q, x].astype(F32)
        for n in range(NX - 1):
            cols = cols + col_last[q, n].astype(F32)
        total = jnp.concatenate([rows, cols], axis=0)
        score = score_sum[q]
        for n in range(len(plane)):
            score = score + score_recv[q, n]
        high = score.astype(BF16)
        rest = score - high.astype(F32)
        middle = rest.astype(BF16)
        low_bits = (rest - middle.astype(F32)).astype(BF16)
        message = dot(spread, total.astype(BF16), ((1,), (0,)))
        for n, piece in enumerate((high, middle, low_bits)):
            message = jnp.where(back_row == CAP + n, piece.astype(F32), message)
        message = message.astype(BF16)
        back_send[pl.ds(q * GROUP * BACK, GROUP * BACK), :] = message
        if q == 0:
            back_recv[0:BACK, :] = message[:BACK]
        for place in range(q * GROUP, (q + 1) * GROUP):
            if place:
                send(
                    back_send.at[pl.ds(place * BACK, BACK), :],
                    back_recv.at[pl.ds(opposite(place) * BACK, BACK), :],
                    8,
                    sem_back,
                    at_z(offset_of(place)),
                )

    def weight_in(begin, end):
        def step(b, _):
            x_rows = x_all[b // NX, b % NX]
            full = dot(x_rows, grads[...], ((0,), (0,)))
            at = pl.ds(pl.multiple_of(b * LANES, LANES), LANES)
            gate_full[0, at, :] = full[:, :LANES].astype(BF16)
            up_full[0, at, :] = full[:, LANES:].astype(BF16)
            for h in range(2):
                piece = full[:, h * LANES : (h + 1) * LANES]
                norms[h : h + 1, at] = jnp.sum(
                    jnp.transpose(piece * piece), axis=0, keepdims=True
                )
            return 0

        lax.fori_loop(begin, end, step, 0)
        if end == NT:
            for n, (dy, dx) in enumerate(plane):
                send(norms, norms_recv.at[n], 9, sem_norm, at_plane(dy, dx))

    def weight_down():
        hidden_t = jnp.transpose(hidden_all[...].astype(F32)).astype(BF16)

        def step(b, squares):
            y_rows = jnp.concatenate(
                [y_all[b // 2, 2 * (b % 2)], y_all[b // 2, 2 * (b % 2) + 1]], axis=1
            )
            full = dot(hidden_t, y_rows, ((1,), (0,)))
            at = pl.ds(pl.multiple_of(b * 2 * LANES, 2 * LANES), 2 * LANES)
            down_full[0, :, at] = full.astype(BF16)
            left, right = full[:, :LANES], full[:, LANES:]
            return squares + left * left + right * right

        squares = lax.fori_loop(0, NT // 2, step, jnp.zeros((LANES, LANES), F32))
        down_norms_out[...] = jnp.sum(jnp.transpose(squares), axis=0, keepdims=True)

    stages = dict(
        A=stage_gather_first,
        B=stage_gather_second,
        G=stage_forward,
        C=stage_cores,
        D=stage_compute,
        E=stage_pair_sum,
        H=stage_reduce,
        F=stage_back,
        R=stage_relay,
    )
    for name, q in ORDER:
        stages[name](int(q))
    weight_down()
    stage_reduce(NQ - 2)
    stage_back(NQ - 3)
    weight_in(0, NT // 4)
    stage_reduce(NQ - 1)
    stage_back(NQ - 2)
    weight_in(NT // 4, 5 * NT // 8)
    stage_back(NQ - 1)
    weight_in(5 * NT // 8, NT)

    await_bytes(back_recv.at[pl.ds(BACK, (NZ - 1) * BACK), :], sem_back)
    rows_back = iota((NZ * BACK, block), 0)
    returned = back_recv[...]
    row_hot = None
    for k in range(2):
        start = places[k] * BACK
        hot = rows_back == start + slots[k]
        row_hot = hot if row_hot is None else row_hot | hot
        score_hot = (rows_back >= start + CAP) & (rows_back < start + CAP + 3)
        mirrored = jnp.where(
            (places[k] == 0) | (places[k] == NZ - 1),
            places[k],
            jnp.where(places[k] % 2 == 1, places[k] + 1, places[k] - 1),
        )
        lane = mirrored % GROUP * CAP + slots[k]
        lines = dot(returned, score_hot.astype(BF16), ((0,), (0,)))
        score = jnp.sum(
            jnp.where(iota((LANES, block), 0) == lane, lines, 0.0), axis=0, keepdims=True
        )
        mixing_out[k : k + 1, :] = score / mixing_rows[k : k + 1, :]
    token_out[...] = dot(row_hot.astype(BF16), returned, ((0,), (0,))).astype(BF16)

    await_bytes(norms_recv, sem_norm)
    total = norms[...]
    for n in range(len(plane)):
        total = total + norms_recv[n]
    norms_out[0] = total

    sent = (
        z_recv.at[pl.ds(tiles, (NZ - 1) * tiles)],
        x_all.at[0, pl.ds(0, 3)],
        x_all.at[pl.ds(0, 2)],
        x_all,
        x_all.at[pl.ds(0, 2)],
        score_in,
        row_recv,
        score_recv,
        back_recv.at[pl.ds(BACK, (NZ - 1) * BACK), :],
        norms_recv,
        z_relay,
        x_all.at[0],
        col_recv,
        row_last,
        col_last,
    )
    for n, ref in enumerate(sent):
        await_bytes(ref, sem_send.at[n])


def write_out(*refs):
    count = len(refs) // 2
    sems = refs[-1]
    copies = [
        pltpu.make_async_copy(refs[n], refs[count + n], sems.at[n]) for n in range(count)
    ]
    for copy in copies:
        copy.start()
    for copy in copies:
        copy.wait()


def on_device(tokens, routing, mixing, gate_matrix, up_matrix, down_matrix, upstream):
    vmem = pl.BlockSpec(memory_space=pltpu.VMEM)
    hbm = pl.BlockSpec(memory_space=pltpu.HBM)
    block = tokens.shape[0]
    shape = jax.ShapeDtypeStruct
    dma = pltpu.SemaphoreType.DMA
    shapes = (
        shape((block, LANES), BF16),
        shape((2, block), F32),
        shape(gate_matrix.shape, BF16),
        shape(up_matrix.shape, BF16),
        shape(down_matrix.shape, BF16),
        shape((1, 2, NT * LANES), F32),
        shape((1, LANES), F32),
    )
    results = pl.pallas_call(
        body,
        out_shape=tuple(pltpu.VMEM(s.shape, s.dtype) for s in shapes),
        in_specs=[hbm] * 7,
        out_specs=[vmem] * 7,
        scratch_shapes=[
            pltpu.VMEM((block, LANES), BF16),
            pltpu.VMEM((block, LANES), BF16),
            pltpu.VMEM((2, block), jnp.int32),
            pltpu.VMEM((2, block), F32),
            pltpu.VMEM((NT * LANES, 2 * LANES), BF16),
            pltpu.VMEM((LANES, NT * LANES), BF16),
            pltpu.VMEM((NZ * SEND // 8, 8, LANES), BF16),
            pltpu.VMEM((NZ * SEND // 8, 8, LANES), BF16),
            pltpu.VMEM(((NZ - FAR) * SEND // 8, 8, LANES), BF16),
            pltpu.VMEM((NY, NX, ALL, LANES), BF16),
            pltpu.VMEM((NY, NX, ALL, LANES), BF16),
            pltpu.VMEM((ALL, 2 * LANES), BF16),
            pltpu.VMEM((ALL, LANES), BF16),
            pltpu.VMEM((NY, NX, ALL, LANES), BF16),
            pltpu.VMEM((NQ, NY, NX, HALF, LANES), BF16),
            pltpu.VMEM((NQ, NY, NX, HALF, LANES), BF16),
            pltpu.VMEM((NQ, NX - 1, NY, SPLIT, LANES), BF16),
            pltpu.VMEM((NQ, NY - 1, NX, HALF - SPLIT, LANES), BF16),
            pltpu.VMEM((NQ, NY, SPLIT, LANES), BF16),
            pltpu.VMEM((NQ, NX, HALF - SPLIT, LANES), BF16),
            pltpu.VMEM((NQ, NY - 1, SPLIT, LANES), BF16),
            pltpu.VMEM((NQ, NX - 1, HALF - SPLIT, LANES), BF16),
            pltpu.VMEM((NQ, 2, 1, LANES), F32),
            pltpu.VMEM((NQ, 1, LANES), F32),
            pltpu.VMEM((NQ, 1, LANES), F32),
            pltpu.VMEM((NQ, NT - 1, 1, LANES), F32),
            pltpu.VMEM((NZ * BACK, LANES), BF16),
            pltpu.VMEM((NZ * BACK, LANES), BF16),
            pltpu.VMEM((2, NT * LANES), F32),
            pltpu.VMEM((NT - 1, 2, NT * LANES), F32),
            dma((4,)),
            dma((3,)),
            dma((15,)),
            dma((NQ,)),
            dma((NQ // 2,)),
            dma((NQ, 2, 3)),
            dma((NQ, 2, 2)),
            dma((NQ, 2, 2)),
            dma((NQ, 2)),
            dma((NQ,)),
            dma((NQ,)),
            dma((NQ,)),
            dma((NQ,)),
            dma((NQ,)),
            dma((NQ,)),
            dma((NQ,)),
            dma,
            dma,
        ],
        compiler_params=pltpu.CompilerParams(
            collective_id=0, has_side_effects=True, vmem_limit_bytes=56 * 1024 * 1024
        ),
    )(
        tokens,
        upstream,
        routing.T,
        mixing.T,
        gate_matrix,
        up_matrix,
        down_matrix,
    )
    results = pl.pallas_call(
        write_out,
        out_shape=shapes,
        in_specs=[vmem] * 7,
        out_specs=[hbm] * 7,
        scratch_shapes=[dma((7,))],
    )(*(pltpu.with_memory_space_constraint(r, pltpu.VMEM) for r in results))
    token_gradient, mixing_t, gate, up, down, norms, down_norms = results
    return token_gradient, mixing_t.T, gate, up, down, norms, down_norms


def solution(mesh):
    placed = (
        P("ep", "tp"),
        P("ep", None),
        P("ep", None),
        P("ep", None, "tp"),
        P("ep", None, "tp"),
        P("ep", "tp", None),
        P("ep", "tp"),
    )
    return jax.shard_map(
        on_device,
        mesh=mesh,
        in_specs=placed,
        out_specs=(
            P("ep", "tp"),
            P("ep", None),
            P("ep", None, "tp"),
            P("ep", None, "tp"),
            P("ep", "tp", None),
            P("ep", None, None),
            P("ep", "tp"),
        ),
        check_vma=False,
    )
```
